128 devices in a mesh: ra: 16 (over z, y), cb: 4 (over x), dp: 2 (over core).
Axes of the slice: x: 4, y: 4, z: 4, core: 2. Of those that a mesh axis runs over, the one named last changes fastest.
Arguments:
- tokens: bfloat16 [3072, 4096], P('dp', 'ra'), may hold values from -20 to 20
- pre_gain: float32 [4096], P('ra'), may hold values from 0.1 to 1.9
- up_weight: bfloat16 [4096, 16384], P('ra', 'cb'), may hold values from -0.09375 to 0.09375
- up_bias: float32 [16384], P('cb'), may hold values from -4 to 4
- down_weight: bfloat16 [16384, 4096], P('cb', 'ra'), may hold values from -0.046875 to 0.046875
- post_gain: float32 [4096], P('ra'), may hold values from 0.1 to 1.9
Outputs:
- stream_out: bfloat16 [3072, 4096], P('dp', 'ra')
The draws below stay inside these ranges and needn't reach their ends.
All inputs are finite; a program needn't handle non-finite values.
Results may differ from the reference program's by a relative error of at most 0.0051.
Values may be sent and summed in bfloat16 or wider, within the bound.
A program may use at most 128 MiB of HBM per device.

```python
import jax
import jax.numpy as jnp
from jax import lax

D = 4096
FF = 16384
TOKENS = 3072


def draw_tokens(key, part):
    first, second, third = jax.random.split(key, 3)
    column = jnp.exp(jax.random.uniform(second, (D // 16,), jnp.float32, -1.2, 1.2))
    column = jnp.repeat(column, 16)
    values = jax.random.normal(first, (TOKENS, D), jnp.float32) * column
    return jnp.clip(values, -20.0, 20.0).astype(jnp.bfloat16)


def block_scale(rng, shape, cuts, low, largest):
    gain = 1.0
    for axis_at, shards_of in cuts:
        draws = jax.random.uniform(jax.random.fold_in(jax.random.fold_in(rng, 6), axis_at), (shards_of,), jnp.float32, low / len(cuts), largest / len(cuts))
        gain = gain * jnp.repeat(jnp.exp(draws), shape[axis_at] // shards_of).reshape((-1,) + (1,) * (len(shape) - 1 - axis_at))
    return gain


def bell_draw(own_key, shape, deviation, limit, shards=(), held_as=jnp.bfloat16):
    drawn = jax.random.normal(own_key, shape, jnp.float32) * deviation
    if len(shards) > 0:
        drawn = block_scale(own_key, shape, shards, -0.22, 0.18) * drawn
    return jnp.clip(drawn, min=-limit, max=limit).astype(held_as)


def setup_inputs(seed: int = 0) -> dict:
    seeds = jax.random.split(jax.random.key(seed), 7)
    return {
        "tokens": draw_tokens(jax.random.fold_in(seeds[6], 71), 0),
        "pre_gain": jnp.clip(1.0 + 0.18 * jax.random.normal(seeds[1], (D,), jnp.float32), 0.1, 1.9),
        "up_weight": bell_draw(seeds[2], (D, FF), D ** -0.5, 0.09375, ((0, 16), (1, 4))),
        "up_bias": bell_draw(seeds[3], (FF,), 1.0, 4.0, ((0, 4),), jnp.float32),
        "down_weight": bell_draw(seeds[4], (FF, D), FF ** -0.5, 0.046875, ((0, 4), (1, 16))),
        "post_gain": jnp.clip(1.0 + 0.18 * jax.random.normal(seeds[5], (D,), jnp.float32), 0.1, 1.9),
    }


epsilon = 1e-06
residual_weight = 0.5

def reference(tokens, pre_gain, up_weight, up_bias, down_weight, post_gain):
    stream = tokens.astype(jnp.float32)
    energy = lax.optimization_barrier(jnp.sum(stream * stream, axis=1))
    inverse = lax.rsqrt(energy / D + epsilon)
    scaled = (stream * pre_gain).astype(jnp.bfloat16)
    pre = jnp.dot(scaled, up_weight, preferred_element_type=jnp.float32) * inverse[:, None] + up_bias
    hidden = jnp.square(jax.nn.relu(pre)).astype(jnp.bfloat16)
    branch = jnp.dot(hidden, down_weight, preferred_element_type=jnp.float32)
    branch_energy = lax.optimization_barrier(jnp.sum(branch * branch, axis=1))
    normed = branch * lax.rsqrt(branch_energy / D + epsilon)[:, None] * post_gain
    return (residual_weight * stream + normed).astype(jnp.bfloat16)
```

```python
import functools

import jax
import jax.numpy as jnp
from jax import lax
from jax.experimental import pallas as pl
from jax.experimental.pallas import tpu as pltpu
from jax.sharding import PartitionSpec as P

MESH = pl.DeviceIdType.MESH
D = 4096
CHUNKS = 6
epsilon = 1e-06
residual_weight = 0.5
f32, bf16 = jnp.float32, jnp.bfloat16


def lane_sums_as_row(square):
    ones = jnp.ones((8, square.shape[1]), bf16)
    high = square.astype(bf16)
    low = (square - high.astype(f32)).astype(bf16)
    contract = (((1,), (1,)), ((), ()))
    total = lax.dot_general(ones, high, contract, preferred_element_type=f32)
    return total + lax.dot_general(ones, low, contract, preferred_element_type=f32)


def kernel(
    tok, pre_gain, up_bias, post_gain, up_hbm, down_hbm, out,
    xg, wu, wd, ps, pr, hg, os, zr, xs, xr, br, inv_col,
    e_own, e_in, be, be_in,
    ssem, rsem, wssem, wrsem, lsem,
):
    C, _, Q, _ = tok.shape
    R = 4 * Q
    ra, x, k = lax.axis_index("ra"), lax.axis_index("cb"), lax.axis_index("dp")
    z, y = ra // 4, ra % 4

    def peer(axis, j):
        if axis == "z":
            return {"ra": ((z + j) % 4) * 4 + y}
        if axis == "y":
            return {"ra": z * 4 + (y + j) % 4}
        if axis == "x":
            return {"cb": (x + j) % 4}
        return {"dp": 1 - k}

    def rdma(src, dst, ss, rs, axis, j):
        return pltpu.make_async_remote_copy(
            src_ref=src, dst_ref=dst, send_sem=ss, recv_sem=rs, device_id=peer(axis, j), device_id_type=MESH
        )

    def cols(at):
        return pl.ds(pl.multiple_of(at * 256, 256), 256)

    phases = {
        "xz": (0, "z", lambda c, j: xg.at[c, x, :, cols(z)], lambda c, j: xg.at[c, x, :, cols(z)], lambda c, j: xg.at[c, x, :, cols((z + 4 - j) % 4)]),
        "xx": (1, "x", lambda c, j: xg.at[c, x], lambda c, j: xg.at[c, x], lambda c, j: xg.at[c, (x + 4 - j) % 4]),
        "yr": (2, "y", lambda c, j: ps.at[c, (y + j) % 4], lambda c, j: pr.at[c, j - 1], lambda c, j: pr.at[c, j - 1]),
        "ya": (3, "y", lambda c, j: hg.at[c, y], lambda c, j: hg.at[c, y], lambda c, j: hg.at[c, (y + 4 - j) % 4]),
        "zr": (4, "z", lambda c, j: os.at[c, (z + j) % 4], lambda c, j: zr.at[c, j - 1], lambda c, j: zr.at[c, j - 1]),
        "xr": (5, "x", lambda c, j: xs.at[c, (x + j) % 4], lambda c, j: xr.at[c, j - 1], lambda c, j: xr.at[c, j - 1]),
        "ez": (6, "z", lambda c, j: be.at[0, c], lambda c, j: be_in.at[0, c, j - 1], lambda c, j: be_in.at[0, c, j - 1]),
        "ey": (7, "y", lambda c, j: be.at[1, c], lambda c, j: be_in.at[1, c, j - 1], lambda c, j: be_in.at[1, c, j - 1]),
        "xo": (8, "x", lambda c, j: out.at[c, x], lambda c, j: out.at[c, x], lambda c, j: out.at[c, (x + 4 - j) % 4]),
    }

    def copy(name, c, j, landing=False):
        n, axis, src, dst, land = phases[name]
        return rdma(src(c, j), (land if landing else dst)(c, j), ssem.at[n, c, j - 1], rsem.at[n, c, j - 1], axis, j)

    def send(name, c):
        for j in (1, 3, 2):
            copy(name, c, j).start()

    def arrived(name, c):
        for j in (1, 3, 2):
            copy(name, c, j, True).wait_recv()

    def up_block(j):
        return rdma(
            up_hbm.at[pl.ds(pl.multiple_of(k * 128, 128), 128), pl.ds(pl.multiple_of(((z + j) % 4) * 1024, 1024), 1024)],
            wu.at[z, k], wssem.at[0, j - 1], wrsem.at[0, j - 1], "z", j,
        )

    def down_block(j):
        return rdma(
            down_hbm.at[pl.ds(pl.multiple_of(((z + j) % 4) * 1024 + k * 512, 512), 512), :],
            wd.at[z, k], wssem.at[1, j - 1], wrsem.at[1, j - 1], "z", j,
        )

    def got(w, n, j):
        at = w.at[(z + 4 - j) % 4, k]
        return rdma(at, at, wssem.at[n, j - 1], wrsem.at[n, j - 1], "z", j)

    def hand(w, n, j, half):
        at = w.at[(z + 4 - j) % 4, half]
        return rdma(at, at, wssem.at[n + 2, j - 1], wrsem.at[n + 2, j - 1], "k", 0)

    def e_copy(n, j):
        return rdma(e_own.at[n], e_in.at[n, j - 1], wssem.at[4 + n, j - 1], wrsem.at[4 + n, j - 1], "zy"[n], j)

    barrier = pltpu.get_barrier_semaphore()
    partners = [(axis, j) for axis in "xyz" for j in (1, 2, 3)] + [("k", 0)]
    for axis, j in partners:
        pl.semaphore_signal(barrier, inc=1, device_id=peer(axis, j), device_id_type=MESH)

    own = []
    for half in range(2):
        own.append(pltpu.make_async_copy(
            up_hbm.at[pl.ds(half * 128, 128), pl.ds(pl.multiple_of(z * 1024, 1024), 1024)], wu.at[z, half], lsem.at[half]))
        own.append(pltpu.make_async_copy(
            down_hbm.at[pl.ds(pl.multiple_of(z * 1024 + half * 512, 512), 512), :], wd.at[z, half], lsem.at[2 + half]))
    for o in own:
        o.start()

    gain = pre_gain[...]

    def scale(c, _):
        xg[c, x, :, cols(z)] = (tok[c, x].astype(f32) * gain).astype(bf16)
        return 0

    lax.fori_loop(0, C, scale, 0)
    pl.semaphore_wait(barrier, len(partners))

    send("xz", 0)
    for j in (1, 3, 2):
        up_block(j).start()
    lax.fori_loop(1, C, lambda c, _: (send("xz", c), 0)[1], 0)
    for j in (1, 3, 2):
        down_block(j).start()

    def own_energy(c, _):
        part = tok[c].reshape(R, 256).astype(f32)
        e_own[0, c] = lane_sums_as_row(part * part)
        return 0

    lax.fori_loop(0, C, own_energy, 0)
    for j in (1, 3, 2):
        e_copy(0, j).start()

    def relay(c, _):
        arrived("xz", c)
        send("xx", c)
        return 0

    relay(0, 0)
    for j in (1, 3, 2):
        got(wu, 0, j).wait_recv()
        hand(wu, 0, j, k).start()
    lax.fori_loop(1, C, relay, 0)
    for j in (1, 3, 2):
        e_copy(0, j).wait_recv()
    e_own[1] = e_own[0] + e_in[0, 0] + e_in[0, 1] + e_in[0, 2]
    for j in (1, 3, 2):
        e_copy(1, j).start()
    for j in (1, 3, 2):
        e_copy(1, j).wait_recv()
    for c in range(C):
        total = e_own[1, c] + e_in[1, 0, c] + e_in[1, 1, c] + e_in[1, 2, c]
        inverse = lax.rsqrt(total / D + epsilon)
        inv_col[c] = jnp.transpose(inverse).reshape(4, Q, 8)
    for o in own:
        o.wait()
    for j in (1, 3, 2):
        hand(wu, 0, j, 1 - k).wait_recv()

    def up(c):
        arrived("xx", c)
        rows = xg[c].reshape(R, 1024)
        for n in range(4):
            w = wu[:, :, :, n * 256 : (n + 1) * 256].reshape(1024, 256)
            part = jnp.dot(rows, w, preferred_element_type=f32)
            ps[c, :, :, n * 256 : (n + 1) * 256] = part.reshape(4, Q, 256).astype(bf16)
        send("yr", c)

    def activate(c):
        arrived("yr", c)
        inverse = inv_col[c, y][:, 0:1]
        for n in range(4):
            at = slice(n * 256, (n + 1) * 256)
            pre = ps[c, y, :, at].astype(f32)
            for j in range(3):
                pre = pre + pr[c, j, :, at].astype(f32)
            pre = pre * inverse + up_bias[z, :, at]
            hg[c, y, :, at] = jnp.square(jnp.maximum(pre, 0.0)).astype(bf16)
        send("ya", c)

    def down(c):
        arrived("ya", c)
        rows = hg[c].reshape(R, 1024)
        for n in range(4):
            os[c, n] = jnp.dot(rows, wd[n].reshape(1024, 256), preferred_element_type=f32).astype(bf16)
        send("zr", c)

    def sum_z(c):
        arrived("zr", c)
        total = os[c, z].astype(f32)
        for j in range(3):
            total = total + zr[c, j].astype(f32)
        xs[c] = total.reshape(4, Q, 256).astype(bf16)
        send("xr", c)

    def sum_x(c):
        arrived("xr", c)
        total = xs[c, x].astype(f32)
        for j in range(3):
            total = total + xr[c, j].astype(f32)
        br[c] = total
        be[0, c] = lane_sums_as_row(total * total)
        send("ez", c)

    def energy_y(c):
        arrived("ez", c)
        be[1, c] = be[0, c] + be_in[0, c, 0] + be_in[0, c, 1] + be_in[0, c, 2]
        send("ey", c)

    def finish(c):
        arrived("ey", c)
        total = be[1, c] + be_in[1, c, 0] + be_in[1, c, 1] + be_in[1, c, 2]
        inverse = jnp.transpose(lax.rsqrt(total / D + epsilon))[:, 0:1]
        normed = br[c] * inverse * post_gain[...]
        out[c, x] = (residual_weight * tok[c, x].astype(f32) + normed).astype(bf16)
        send("xo", c)

    stages = (up, activate, down, sum_z, sum_x, energy_y, finish)

    def step(s, _):
        for depth, stage in enumerate(stages):
            if depth == 2:
                @pl.when(s == 2)
                def _():
                    for j in (1, 3, 2):
                        got(wd, 1, j).wait_recv()
                        hand(wd, 1, j, k).start()
                    for j in (1, 3, 2):
                        hand(wd, 1, j, 1 - k).wait_recv()

            pl.when((s >= depth) & (s < C + depth))(lambda stage=stage, depth=depth: stage(s - depth))
        return 0

    lax.fori_loop(0, C + len(stages) - 1, step, 0)

    def close(c, _):
        arrived("xo", c)
        for name in phases:
            for j in (1, 2, 3):
                copy(name, c, j).wait_send()
        return 0

    lax.fori_loop(0, C, close, 0)
    for j in (1, 2, 3):
        up_block(j).wait_send()
        down_block(j).wait_send()
        hand(wu, 0, j, k).wait_send()
        hand(wd, 1, j, k).wait_send()
        e_copy(0, j).wait_send()
        e_copy(1, j).wait_send()


def body(tokens, pre_gain, up_weight, up_bias, down_weight, post_gain):
    C = CHUNKS
    T = tokens.shape[0]
    R = T // C
    Q = R // 4
    vmem = pl.BlockSpec(memory_space=pltpu.VMEM)
    hbm = pl.BlockSpec(memory_space=pl.ANY)
    dma = pltpu.SemaphoreType.DMA
    result = pl.pallas_call(
        kernel,
        out_shape=jax.ShapeDtypeStruct((C, 4, Q, 256), bf16),
        in_specs=[vmem, vmem, vmem, vmem, hbm, hbm],
        out_specs=vmem,
        scratch_shapes=[
            pltpu.VMEM((C, 4, Q, 1024), bf16),
            pltpu.VMEM((4, 2, 128, 1024), bf16),
            pltpu.VMEM((4, 2, 512, 256), bf16),
            pltpu.VMEM((C, 4, Q, 1024), bf16),
            pltpu.VMEM((C, 3, Q, 1024), bf16),
            pltpu.VMEM((C, 4, Q, 1024), bf16),
            pltpu.VMEM((C, 4, R, 256), bf16),
            pltpu.VMEM((C, 3, R, 256), bf16),
            pltpu.VMEM((C, 4, Q, 256), bf16),
            pltpu.VMEM((C, 3, Q, 256), bf16),
            pltpu.VMEM((C, Q, 256), f32),
            pltpu.VMEM((C, 4, Q, 8), f32),
            pltpu.VMEM((2, C, 8, R), f32),
            pltpu.VMEM((2, 3, C, 8, R), f32),
            pltpu.VMEM((2, C, 8, Q), f32),
            pltpu.VMEM((2, C, 3, 8, Q), f32),
            dma((9, C, 3)),
            dma((9, C, 3)),
            dma((6, 3)),
            dma((6, 3)),
            dma((4,)),
        ],
        compiler_params=pltpu.CompilerParams(
            collective_id=0, has_side_effects=True, vmem_limit_bytes=56 * 2**20
        ),
    )(
        tokens.reshape(C, 4, Q, 256),
        pre_gain.reshape(1, 256),
        up_bias.reshape(4, 1, 1024),
        post_gain.reshape(1, 256),
        up_weight,
        down_weight,
    )
    return result.reshape(T, 256)


def solution(mesh):
    in_specs = (P("dp", "ra"), P("ra"), P("ra", "cb"), P("cb"), P("cb", "ra"), P("ra"))
    out_specs = P("dp", "ra")
    return jax.shard_map(body, mesh=mesh, in_specs=in_specs, out_specs=out_specs, check_vma=False)
```

```python
import jax
import jax.numpy as jnp
from jax import lax
from jax.experimental import pallas as pl
from jax.experimental.pallas import tpu as pltpu
from jax.sharding import PartitionSpec as P

MESH = pl.DeviceIdType.MESH
D = 4096
CHUNKS = 12
GROUP = 4
LAG = 2
LATER = (4, 4, 6)
VMEM_LIMIT = 56 * 2**20
epsilon = 1e-06
residual_weight = 0.5
f32, bf16 = jnp.float32, jnp.bfloat16


def lane_sums_as_row(square):
    ones = jnp.ones((8, square.shape[1]), bf16)
    high = square.astype(bf16)
    low = (square - high.astype(f32)).astype(bf16)
    contract = (((1,), (1,)), ((), ()))
    total = lax.dot_general(ones, high, contract, preferred_element_type=f32)
    return total + lax.dot_general(ones, low, contract, preferred_element_type=f32)


def kernel(
    tok_hbm, pre_gain, up_bias, post_gain, up_hbm, down_hbm, out_hbm,
    tok, xg, wu, wd, pf, ps, r1, rs, pr, hg, os, of, zr, xa, inv_row, inv_col, e_own, e_in, be, be_in, out,
    ssem, csem, usem, esem, wssem, wrsem, lsem, osem,
):
    G = GROUP
    C, _, Q, _ = tok.shape
    R = 4 * Q
    ra, x, k = lax.axis_index("ra"), lax.axis_index("cb"), lax.axis_index("dp")
    z, y = ra // 4, ra % 4
    halves = (slice(0, 256), slice(256, 512))

    def peer(axis, j):
        if axis == "r":
            return {"ra": (ra + j) % 16}
        if axis == "z":
            return {"ra": ((z + j) % 4) * 4 + y}
        if axis == "y":
            return {"ra": z * 4 + (y + j) % 4}
        if axis == "x":
            return {"cb": (x + j) % 4}
        return {"dp": 1 - k}

    def rdma(src, dst, ss, rs, axis, j):
        return pltpu.make_async_remote_copy(
            src_ref=src, dst_ref=dst, send_sem=ss, recv_sem=rs, device_id=peer(axis, j), device_id_type=MESH
        )

    def cols(at):
        return pl.ds(pl.multiple_of(at * 256, 256), 256)

    def side(j):
        return 0 if j == 1 else 1

    phases = {
        "xz": (0, "z", (1, 3, 2), lambda c, j: xg.at[c, x, :, cols(z)], lambda c, j: xg.at[c, x, :, cols(z)],
               lambda c: xa.at[c, 0:3, 0:Q]),
        "xx": (1, "x", (1, 3, 2), lambda c, j: xg.at[c, x], lambda c, j: xg.at[c, x], lambda c: xg.at[c, 0:3]),
        "r1": (2, "y", (1, 3), lambda u, j: ps.at[u, (y + 2) % 4, :, halves[side(j)]], lambda u, j: r1.at[u, side(j)],
               lambda u: r1.at[u]),
        "rd": (3, "y", (1, 3), lambda u, j: ps.at[u, (y + j) % 4, :, halves[1 - side(j)]],
               lambda u, j: pr.at[u, side(j), :, halves[1 - side(j)]], lambda u: r1.at[u]),
        "r2": (4, "y", (1, 3), lambda u, j: rs.at[u, side(j)], lambda u, j: pr.at[u, side(j), :, halves[side(j)]],
               lambda u: pr.at[u]),
        "a1": (5, "y", (1, 3), lambda u, j: hg.at[u, y], lambda u, j: hg.at[u, y], lambda u: hg.at[u, 0:2]),
        "a2": (6, "y", (1, 3), lambda u, j: hg.at[u, (y + 4 - j) % 4, :, halves[side(j)]],
               lambda u, j: hg.at[u, (y + 4 - j) % 4, :, halves[side(j)]], lambda u: r1.at[u]),
        "zr": (7, "z", (1, 3, 2), lambda c, j: os.at[c, (z + j) % 4], lambda c, j: zr.at[c, j - 1], lambda c: zr.at[c]),
        "xa": (8, "x", (1, 3, 2), lambda c, j: xa.at[c, x], lambda c, j: xa.at[c, x], lambda c: zr.at[c]),
    }
    sent = {
        "xz": xa.at[:, 0:3, 0:Q], "xx": xg.at[:, 0:3], "r1": r1, "rd": r1, "r2": r1, "a1": hg.at[:, 0:2], "a2": r1, "zr": zr,
        "xa": zr,
    }
    by_chunk = {"xz": 0, "xx": 1, "zr": 2, "xa": 3}
    by_unit = {"r1": 0, "rd": 1, "r2": 1, "a1": 2, "a2": 3}

    def landed(name, i):
        return csem.at[by_chunk[name], i] if name in by_chunk else usem.at[by_unit[name], i]

    def send(name, i):
        n, axis, offsets, src, dst, _ = phases[name]
        for j in offsets:
            rdma(src(i, j), dst(i, j), ssem.at[n], landed(name, i), axis, j).start()

    def arrived(name, i):
        with jax.named_scope("wait_" + name):
            all_of_it = phases[name][5](i)
            pltpu.make_async_copy(all_of_it, all_of_it, landed(name, i)).wait()

    def up_block(h, j):
        at = pl.ds(pl.multiple_of(((z + j) % 4) * 1024 + h * 512, 512), 512)
        return rdma(
            up_hbm.at[pl.ds(pl.multiple_of(k * 128, 128), 128), at], wu.at[h, z, k], wssem.at[h], wrsem.at[h, j - 1], "z", j
        )

    def down_block(j):
        return rdma(
            down_hbm.at[pl.ds(pl.multiple_of(((z + j) % 4) * 1024 + k * 512, 512), 512), :],
            wd.at[z, k], wssem.at[2], wrsem.at[2, j - 1], "z", j,
        )

    def got(w, n, j):
        at = w.at[(z + 4 - j) % 4, k]
        return rdma(at, at, wssem.at[n], wrsem.at[n, j - 1], "z", j)

    def hand(w, n, j, half):
        at = w.at[(z + 4 - j) % 4, half]
        return rdma(at, at, wssem.at[n + 3], wrsem.at[n + 3, j - 1], "k", 0)

    def take(w, n):
        with jax.named_scope("wait_w"):
            for j in (1, 3, 2):
                got(w, n, j).wait_recv()
                hand(w, n, j, k).start()

    def have(w, n):
        with jax.named_scope("wait_hand"):
            for j in (1, 3, 2):
                hand(w, n, j, 1 - k).wait_recv()

    def send_energy(n):
        for j in (1, 3, 2):
            rdma(e_own.at[n], e_in.at[n, j - 1], esem.at[n], esem.at[2 + n], "zy"[n], j).start()

    def have_energy(n):
        with jax.named_scope("wait_e"):
            pltpu.make_async_copy(e_in.at[n], e_in.at[n], esem.at[2 + n]).wait()
        return e_own[n] + e_in[n, 0] + e_in[n, 1] + e_in[n, 2]

    def send_rows(c):
        for j in range(1, 16):
            rdma(be.at[c], be_in.at[c, j - 1], esem.at[4], esem.at[5 + c], "r", j).start()

    load = pltpu.make_async_copy(tok_hbm, tok, lsem.at[6])
    load.start()
    barrier = pltpu.get_barrier_semaphore()
    partners = [(axis, j) for axis in "xyz" for j in (1, 2, 3)] + [("k", 0)]
    for axis, j in partners:
        pl.semaphore_signal(barrier, inc=1, device_id=peer(axis, j), device_id_type=MESH)

    own = []
    for half in range(2):
        for h in range(2):
            own.append(pltpu.make_async_copy(
                up_hbm.at[pl.ds(half * 128, 128), pl.ds(pl.multiple_of(z * 1024 + h * 512, 512), 512)],
                wu.at[h, z, half], lsem.at[half * 2 + h]))
        own.append(pltpu.make_async_copy(
            down_hbm.at[pl.ds(pl.multiple_of(z * 1024 + half * 512, 512), 512), :], wd.at[z, half], lsem.at[4 + half]))
    for o in own:
        o.start()
    load.wait()

    gain = pre_gain[...]

    def scale(c, _):
        xg[c, x, :, cols(z)] = (tok[c, x].astype(f32) * gain).astype(bf16)
        part = tok[c].reshape(R, 256).astype(f32)
        e_own[0, c] = lane_sums_as_row(part * part)[0:1]
        return 0

    with jax.named_scope("scale"):
        lax.fori_loop(0, C, scale, 0)
    with jax.named_scope("wait_barrier"):
        pl.semaphore_wait(barrier, len(partners))

    early = max(G, C // 2)
    for c in range(2):
        send("xz", c)
    for j in (1, 3, 2):
        up_block(0, j).start()
    send_energy(0)
    for c in range(2, early):
        send("xz", c)
    for j in (1, 3, 2):
        up_block(1, j).start()
    lax.fori_loop(early, C, lambda c, _: (send("xz", c), 0)[1], 0)
    for j in (1, 3, 2):
        down_block(j).start()

    def spread(c):
        arrived("xz", c)
        send("xx", c)

    spread(0)
    spread(1)
    take(wu.at[0], 0)
    for o in own:
        o.wait()
    have(wu.at[0], 0)

    def energy_over_z():
        e_own[1] = have_energy(0)
        send_energy(1)

    def energy_over_y():
        inv_row[...] = lax.rsqrt(have_energy(1) / D + epsilon)

        def turn(c, _):
            inv_col[c] = jnp.transpose(jnp.broadcast_to(inv_row[c], (8, R))).reshape(4, Q, 8)
            return 0

        lax.fori_loop(0, C, turn, 0)

    def late(u):
        return (u // (2 * G) + 15) // 16

    def chunk_of(u):
        return late(u) * (u // 2) + (1 - late(u)) * (u % G)

    def half_of(u):
        return late(u) * (u % 2) + (1 - late(u)) * (u // G)

    def up(u):
        c, h = chunk_of(u), half_of(u)
        rows = xg[c].reshape(R, 1024)
        for n in range(2):
            at = slice(n * 256, (n + 1) * 256)
            part = jnp.dot(rows, wu[h, :, :, :, at].reshape(1024, 256), preferred_element_type=f32).reshape(4, Q, 256)
            pf[u, :, :, at] = part
            ps[u, :, :, at] = part.astype(bf16)
        send("r1", u)
        send("rd", u)

    def add_up(u):
        arrived("r1", u)
        for j in (1, 3):
            n = side(j)
            rs[u, n] = (pf[u, (y + j) % 4, :, halves[n]] + r1[u, n].astype(f32)).astype(bf16)
        send("r2", u)

    def activate(u):
        arrived("r2", u)
        inverse = inv_col[chunk_of(u), y][:, 0:1]
        pre = pf[u, y] + pr[u, 0].astype(f32) + pr[u, 1].astype(f32)
        pre = pre * inverse + up_bias[z, half_of(u)]
        hg[u, y] = jnp.square(jnp.maximum(pre, 0.0)).astype(bf16)
        send("a1", u)

    def pass_on(u):
        arrived("a1", u)
        send("a2", u)

    def last_of(u):
        return late(u) * ((u - 1) // 2) + (1 - late(u)) * (u - G)

    def down(u):
        c = last_of(u)
        other = late(u) * (u - 1) + (1 - late(u)) * (u - G)
        for n in range(4):
            part = jnp.dot(hg[other].reshape(R, 512), wd[n, 0], preferred_element_type=f32)
            part = part + jnp.dot(hg[u].reshape(R, 512), wd[n, 1], preferred_element_type=f32)
            of[c, n] = part
            os[c, n] = part.astype(bf16)
        send("zr", c)

    def sum_z(u):
        c = last_of(u)
        arrived("zr", c)
        total = of[c, z]
        for j in range(3):
            total = total + zr[c, j].astype(f32)
        xa[c, x] = total.astype(bf16)
        send("xa", c)

    def branch(c):
        return (xa[c, 0].astype(f32) + xa[c, 1].astype(f32)) + (xa[c, 2].astype(f32) + xa[c, 3].astype(f32))

    def sum_x(u):
        c = last_of(u)
        arrived("xa", c)
        total = branch(c)
        be[c] = lane_sums_as_row(total * total)[0:1]
        send_rows(c)

    def finish(u):
        c = last_of(u)
        with jax.named_scope("wait_be"):
            pltpu.make_async_copy(be_in.at[c], be_in.at[c], esem.at[5 + c]).wait()
        total = be[c]
        for j in range(15):
            total = total + be_in[c, j]
        inverse = jnp.transpose(jnp.broadcast_to(lax.rsqrt(total / D + epsilon), (8, R)))[:, 0:1]
        normed = branch(c) * inverse * post_gain[...]
        out[c] = (residual_weight * tok[c].reshape(R, 256).astype(f32) + normed).astype(bf16)
        pltpu.make_async_copy(out.at[c], out_hbm.at[c], osem.at[c]).start()

    def scoped(stage, u):
        with jax.named_scope(stage.__name__):
            stage(u)

    lag = LAG
    to_down = 4 * lag
    to_z = to_down + LATER[0]
    to_x = to_z + LATER[1]
    to_end = to_x + LATER[2]

    def step(s, _):
        def at(stage, depth, ends=False):
            u = s - depth
            now = (u >= 0) & (u < 2 * C)
            if ends:
                now = now & (u >= G) & ((u < 2 * G) | (u % 2 == 1))
            pl.when(now)(lambda: scoped(stage, u))

        pl.when((s < 2 * C) & ((s < G) | ((s >= 2 * G) & (s % 2 == 0))))(lambda: arrived("xx", chunk_of(s)))
        pl.when(s == G)(lambda: have(wu.at[1], 1))
        at(up, 0)
        pl.when((s + 2 < early))(lambda: scoped(spread, s + 2))
        pl.when(s == lag)(energy_over_z)
        at(add_up, lag)
        pl.when(s == G - 1)(lambda: take(wu.at[1], 1))
        pl.when(s == 2 * lag)(energy_over_y)
        at(activate, 2 * lag)
        pl.when((s >= early) & (s < C))(lambda: scoped(spread, s))
        at(pass_on, 3 * lag)
        pl.when(s == G + to_down - 1)(lambda: take(wd, 2))
        pl.when(s == G + to_down)(lambda: have(wd, 2))
        pl.when((s >= to_down) & (s < 2 * C + to_down))(lambda: arrived("a2", s - to_down))
        at(down, to_down, True)
        at(sum_z, to_z, True)
        at(sum_x, to_x, True)
        at(finish, to_end, True)
        return 0

    lax.fori_loop(0, 2 * C + to_end, step, 0)
    with jax.named_scope("sent"):
        for name, total in sent.items():
            pltpu.make_async_copy(total, total, ssem.at[phases[name][0]]).wait()
        some = wu.at[0, 0:3, 0]
        for n, total in enumerate((some, some, wd.at[0:3, 0], some, some, wd.at[0:3, 0])):
            pltpu.make_async_copy(total, total, wssem.at[n]).wait()
        for n in range(2):
            pltpu.make_async_copy(e_in.at[n], e_in.at[n], esem.at[n]).wait()
        pltpu.make_async_copy(be_in, be_in, esem.at[4]).wait()
        lax.fori_loop(0, C, lambda c, _: (pltpu.make_async_copy(out.at[c], out_hbm.at[c], osem.at[c]).wait(), 0)[1], 0)


def body(tokens, pre_gain, up_weight, up_bias, down_weight, post_gain):
    C = CHUNKS
    T = tokens.shape[0]
    R = T // C
    Q = R // 4
    vmem = pl.BlockSpec(memory_space=pltpu.VMEM)
    hbm = pl.BlockSpec(memory_space=pl.ANY)
    dma = pltpu.SemaphoreType.DMA
    result = pl.pallas_call(
        kernel,
        out_shape=jax.ShapeDtypeStruct((C, R, 256), bf16),
        in_specs=[hbm, vmem, vmem, vmem, hbm, hbm],
        out_specs=hbm,
        scratch_shapes=[
            pltpu.VMEM((C, 4, Q, 256), bf16),
            pltpu.VMEM((C, 4, Q, 1024), bf16),
            pltpu.VMEM((2, 4, 2, 128, 512), bf16),
            pltpu.VMEM((4, 2, 512, 256), bf16),
            pltpu.VMEM((2 * C, 4, Q, 512), f32),
            pltpu.VMEM((2 * C, 4, Q, 512), bf16),
            pltpu.VMEM((2 * C, 2, Q, 256), bf16),
            pltpu.VMEM((2 * C, 2, Q, 256), bf16),
            pltpu.VMEM((2 * C, 2, Q, 512), bf16),
            pltpu.VMEM((2 * C, 4, Q, 512), bf16),
            pltpu.VMEM((C, 4, R, 256), bf16),
            pltpu.VMEM((C, 4, R, 256), f32),
            pltpu.VMEM((C, 3, R, 256), bf16),
            pltpu.VMEM((C, 4, R, 256), bf16),
            pltpu.VMEM((C, 1, R), f32),
            pltpu.VMEM((C, 4, Q, 8), f32),
            pltpu.VMEM((2, C, 1, R), f32),
            pltpu.VMEM((2, 3, C, 1, R), f32),
            pltpu.VMEM((C, 1, R), f32),
            pltpu.VMEM((C, 15, 1, R), f32),
            pltpu.VMEM((C, R, 256), bf16),
            dma((9,)),
            dma((4, C)),
            dma((4, 2 * C)),
            dma((5 + C,)),
            dma((6,)),
            dma((6, 3)),
            dma((7,)),
            dma((C,)),
        ],
        compiler_params=pltpu.CompilerParams(
            collective_id=0, has_side_effects=True, vmem_limit_bytes=VMEM_LIMIT
        ),
    )(
        tokens.reshape(C, 4, Q, 256),
        pre_gain.reshape(1, 256),
        up_bias.reshape(4, 2, 1, 512),
        post_gain.reshape(1, 256),
        up_weight,
        down_weight,
    )
    return result.reshape(T, 256)


def solution(mesh):
    in_specs = (P("dp", "ra"), P("ra"), P("ra", "cb"), P("cb"), P("cb", "ra"), P("ra"))
    out_specs = P("dp", "ra")
    return jax.shard_map(body, mesh=mesh, in_specs=in_specs, out_specs=out_specs, check_vma=False)
```

```python
import jax
import jax.numpy as jnp
from jax import lax
from jax.experimental import pallas as pl
from jax.experimental.pallas import tpu as pltpu
from jax.sharding import PartitionSpec as P

MESH = pl.DeviceIdType.MESH
D = 4096
CHUNKS = 12
GROUP = 5
FIRST = 5
AHEAD = 2
EAGER = 5
LAGS = (2, 2, 2, 2)
LATER = (4, 4, 6)
VMEM_LIMIT = 56 * 2**20
epsilon = 1e-06
residual_weight = 0.5
f32, bf16 = jnp.float32, jnp.bfloat16


def lane_sums_as_row(square):
    ones = jnp.ones((8, square.shape[1]), bf16)
    high = square.astype(bf16)
    low = (square - high.astype(f32)).astype(bf16)
    contract = (((1,), (1,)), ((), ()))
    total = lax.dot_general(ones, high, contract, preferred_element_type=f32)
    return total + lax.dot_general(ones, low, contract, preferred_element_type=f32)


def kernel(
    tok_hbm, pre_gain_hbm, up_bias_hbm, post_gain_hbm, up_hbm, down_hbm, out_hbm,
    tok, pre_gain, up_bias, post_gain, xg, wu, wd, pf, ps, r1, rs, pr, hg, os, of, zr, xa, inv_row, inv_col, e_own, e_in, be, be_in, out,
    ssem, csem, usem, esem, wssem, wrsem, lsem, osem,
):
    G = GROUP
    C, _, Q, _ = tok.shape
    R = 4 * Q
    ra, x, k = lax.axis_index("ra"), lax.axis_index("cb"), lax.axis_index("dp")
    z, y = ra // 4, ra % 4
    halves = (slice(0, 256), slice(256, 512))
    wide = (slice(0, 512), slice(512, 1024))

    def peer(axis, j):
        if axis == "r":
            return {"ra": (ra + j) % 16}
        if axis == "z":
            return {"ra": ((z + j) % 4) * 4 + y}
        if axis == "y":
            return {"ra": z * 4 + (y + j) % 4}
        if axis == "x":
            return {"cb": (x + j) % 4}
        return {"dp": 1 - k}

    def rdma(src, dst, ss, rs, axis, j):
        return pltpu.make_async_remote_copy(
            src_ref=src, dst_ref=dst, send_sem=ss, recv_sem=rs, device_id=peer(axis, j), device_id_type=MESH
        )

    def cols(at):
        return pl.ds(pl.multiple_of(at * 256, 256), 256)

    def side(j):
        return 0 if j == 1 else 1

    phases = {
        "xz": (0, "z", (1, 3, 2), lambda c, j: xg.at[c, x, :, cols(z)], lambda c, j: xg.at[c, x, :, cols(z)],
               lambda c: xa.at[c, 0:3, 0:Q]),
        "xx": (1, "x", (1, 3), lambda c, j: xg.at[c, x], lambda c, j: xg.at[c, x], lambda c: xg.at[c, 0:2]),
        "xf": (9, "x", (1, 3), lambda c, j: xg.at[c, (x + 4 - j) % 4, :, wide[side(j)]],
               lambda c, j: xg.at[c, (x + 4 - j) % 4, :, wide[side(j)]], lambda c: xg.at[c, 0]),
        "r1": (2, "y", (1, 3), lambda u, j: ps.at[u, (y + 2) % 4, :, halves[side(j)]], lambda u, j: r1.at[u, side(j)],
               lambda u: r1.at[u]),
        "rd": (3, "y", (1, 3), lambda u, j: ps.at[u, (y + j) % 4, :, halves[1 - side(j)]],
               lambda u, j: pr.at[u, side(j), :, halves[1 - side(j)]], lambda u: r1.at[u]),
        "r2": (4, "y", (1, 3), lambda u, j: rs.at[u, side(j)], lambda u, j: pr.at[u, side(j), :, halves[side(j)]],
               lambda u: pr.at[u]),
        "a1": (5, "y", (1, 3), lambda u, j: hg.at[u, y], lambda u, j: hg.at[u, y], lambda u: hg.at[u, 0:2]),
        "a2": (6, "y", (1, 3), lambda u, j: hg.at[u, (y + 4 - j) % 4, :, halves[side(j)]],
               lambda u, j: hg.at[u, (y + 4 - j) % 4, :, halves[side(j)]], lambda u: r1.at[u]),
        "zr": (7, "z", (1, 3, 2), lambda c, j: os.at[c, (z + j) % 4], lambda c, j: zr.at[c, j - 1], lambda c: zr.at[c]),
        "xa": (8, "x", (1, 3, 2), lambda c, j: xa.at[c, x], lambda c, j: xa.at[c, x], lambda c: zr.at[c]),
    }
    sent = {
        "xz": xa.at[:, 0:3, 0:Q], "xx": xg.at[:, 0:2], "xf": xg.at[:, 0], "r1": r1, "rd": r1, "r2": r1, "a1": hg.at[:, 0:2],
        "a2": r1, "zr": zr, "xa": zr,
    }
    by_chunk = {"xz": 0, "xx": 1, "zr": 2, "xa": 3, "xf": 4}
    by_unit = {"r1": 0, "rd": 1, "r2": 1, "a1": 0, "a2": 1}

    def landed(name, i):
        return csem.at[by_chunk[name], i] if name in by_chunk else usem.at[by_unit[name], i]

    def send(name, i):
        n, axis, offsets, src, dst, _ = phases[name]
        for j in offsets:
            rdma(src(i, j), dst(i, j), ssem.at[n], landed(name, i), axis, j).start()

    def arrived(name, i):
        with jax.named_scope("wait_" + name):
            all_of_it = phases[name][5](i)
            pltpu.make_async_copy(all_of_it, all_of_it, landed(name, i)).wait()

    def up_block(h, j):
        at = pl.ds(pl.multiple_of(((z + j) % 4) * 1024 + h * 512, 512), 512)
        return rdma(
            up_hbm.at[pl.ds(pl.multiple_of(k * 128, 128), 128), at], wu.at[h, z, k], wssem.at[h], wrsem.at[h, j - 1], "z", j
        )

    def down_block(j):
        return rdma(
            down_hbm.at[pl.ds(pl.multiple_of(((z + j) % 4) * 1024 + k * 512, 512), 512), :],
            wd.at[z, k], wssem.at[2], wrsem.at[2, j - 1], "z", j,
        )

    def got(w, n, j):
        at = w.at[(z + 4 - j) % 4, k]
        return rdma(at, at, wssem.at[n], wrsem.at[n, j - 1], "z", j)

    def hand(w, n, j, half):
        at = w.at[(z + 4 - j) % 4, half]
        return rdma(at, at, wssem.at[n + 3], wrsem.at[n + 3, j - 1], "k", 0)

    def take(w, n):
        with jax.named_scope("wait_w"):
            for j in (1, 3, 2):
                got(w, n, j).wait_recv()
                hand(w, n, j, k).start()

    def have(w, n):
        with jax.named_scope("wait_hand"):
            for j in (1, 3, 2):
                hand(w, n, j, 1 - k).wait_recv()

    def send_energy(n):
        for j in (1, 3, 2):
            rdma(e_own.at[n], e_in.at[n, j - 1], esem.at[n], esem.at[2 + n], "zy"[n], j).start()

    def have_energy(n):
        with jax.named_scope("wait_e"):
            pltpu.make_async_copy(e_in.at[n], e_in.at[n], esem.at[2 + n]).wait()
        return e_own[n] + e_in[n, 0] + e_in[n, 1] + e_in[n, 2]

    def send_rows(c):
        for j in range(1, 16):
            rdma(be.at[c], be_in.at[c, j - 1], esem.at[4], esem.at[5 + c], "r", j).start()

    barrier = pltpu.get_barrier_semaphore()
    partners = [(axis, j) for axis in "xyz" for j in (1, 2, 3)] + [("k", 0)]
    for axis, j in partners:
        pl.semaphore_signal(barrier, inc=1, device_id=peer(axis, j), device_id_type=MESH)

    load = pltpu.make_async_copy(tok_hbm, tok, lsem.at[6])
    load.start()
    small = []
    for n, (far, near) in enumerate(((pre_gain_hbm, pre_gain), (up_bias_hbm, up_bias), (post_gain_hbm, post_gain))):
        small.append(pltpu.make_async_copy(far, near, lsem.at[7 + n]))
        small[-1].start()
    own = []
    for half in range(2):
        for h in range(2):
            own.append(pltpu.make_async_copy(
                up_hbm.at[pl.ds(half * 128, 128), pl.ds(pl.multiple_of(z * 1024 + h * 512, 512), 512)],
                wu.at[h, z, half], lsem.at[half * 2 + h]))
        own.append(pltpu.make_async_copy(
            down_hbm.at[pl.ds(pl.multiple_of(z * 1024 + half * 512, 512), 512), :], wd.at[z, half], lsem.at[4 + half]))
    for o in own:
        o.start()
    load.wait()
    for o in small:
        o.wait()

    gain = pre_gain[...]

    def scale(c, _):
        xg[c, x, :, cols(z)] = (tok[c, x].astype(f32) * gain).astype(bf16)
        return 0

    def own_energy(c, _):
        part = tok[c].reshape(R, 256).astype(f32)
        e_own[0, c] = lane_sums_as_row(part * part)[0:1]
        return 0

    with jax.named_scope("scale"):
        lax.fori_loop(0, C, scale, 0)
    with jax.named_scope("wait_barrier"):
        pl.semaphore_wait(barrier, len(partners))

    early = max(G, C // 2)
    for c in range(FIRST):
        send("xz", c)
    for j in (1, 3, 2):
        up_block(0, j).start()
    with jax.named_scope("own_energy"):
        lax.fori_loop(0, C, own_energy, 0)
    send_energy(0)
    for c in range(FIRST, early):
        send("xz", c)
    for j in (1, 3, 2):
        up_block(1, j).start()
    lax.fori_loop(early, C, lambda c, _: (send("xz", c), 0)[1], 0)
    for j in (1, 3, 2):
        down_block(j).start()

    def spread(c):
        arrived("xz", c)
        send("xx", c)

    def forward(c):
        arrived("xx", c)
        send("xf", c)

    for c in range(FIRST):
        spread(c)
    for c in range(AHEAD):
        forward(c)
    take(wu.at[0], 0)
    for c in range(FIRST, G):
        spread(c)
    for c in range(AHEAD, EAGER):
        forward(c)
    for o in own:
        o.wait()
    have(wu.at[0], 0)

    def energy_over_z():
        e_own[1] = have_energy(0)
        send_energy(1)

    def energy_over_y():
        inv_row[...] = lax.rsqrt(have_energy(1) / D + epsilon)


    def turn(c):
        inv_col[c] = jnp.transpose(jnp.broadcast_to(inv_row[c], (8, R))).reshape(4, Q, 8)

    def late(u):
        return (u // (2 * G) + 15) // 16

    def chunk_of(u):
        return late(u) * (u // 2) + (1 - late(u)) * (u % G)

    def half_of(u):
        return late(u) * (u % 2) + (1 - late(u)) * (u // G)

    def up(u):
        c, h = chunk_of(u), half_of(u)
        rows = xg[c].reshape(R, 1024)
        for n in range(2):
            at = slice(n * 256, (n + 1) * 256)
            part = jnp.dot(rows, wu[h, :, :, :, at].reshape(1024, 256), preferred_element_type=f32).reshape(4, Q, 256)
            pf[u, :, :, at] = part
            ps[u, :, :, at] = part.astype(bf16)
        send("r1", u)
        send("rd", u)

    def add_up(u):
        arrived("r1", u)
        for j in (1, 3):
            n = side(j)
            rs[u, n] = (pf[u, (y + j) % 4, :, halves[n]] + r1[u, n].astype(f32)).astype(bf16)
        send("r2", u)

    def activate(u):
        arrived("r2", u)
        inverse = inv_col[chunk_of(u), y][:, 0:1]
        pre = pf[u, y] + pr[u, 0].astype(f32) + pr[u, 1].astype(f32)
        pre = pre * inverse + up_bias[z, half_of(u)]
        hg[u, y] = jnp.square(jnp.maximum(pre, 0.0)).astype(bf16)
        send("a1", u)

    def pass_on(u):
        arrived("a1", u)
        send("a2", u)

    def last_of(u):
        return late(u) * ((u - 1) // 2) + (1 - late(u)) * (u - G)

    def down(u):
        c = last_of(u)
        other = late(u) * (u - 1) + (1 - late(u)) * (u - G)
        for n in range(4):
            part = jnp.dot(hg[other].reshape(R, 512), wd[n, 0], preferred_element_type=f32)
            part = part + jnp.dot(hg[u].reshape(R, 512), wd[n, 1], preferred_element_type=f32)
            of[c, n] = part
            os[c, n] = part.astype(bf16)
        send("zr", c)

    def sum_z(u):
        c = last_of(u)
        arrived("zr", c)
        total = of[c, z]
        for j in range(3):
            total = total + zr[c, j].astype(f32)
        xa[c, x] = total.astype(bf16)
        send("xa", c)

    def branch(c):
        return (xa[c, 0].astype(f32) + xa[c, 1].astype(f32)) + (xa[c, 2].astype(f32) + xa[c, 3].astype(f32))

    def sum_x(u):
        c = last_of(u)
        arrived("xa", c)
        total = branch(c)
        be[c] = lane_sums_as_row(total * total)[0:1]
        send_rows(c)

    def finish(u):
        c = last_of(u)
        with jax.named_scope("wait_be"):
            pltpu.make_async_copy(be_in.at[c], be_in.at[c], esem.at[5 + c]).wait()
        total = be[c]
        for j in range(15):
            total = total + be_in[c, j]
        inverse = jnp.transpose(jnp.broadcast_to(lax.rsqrt(total / D + epsilon), (8, R)))[:, 0:1]
        normed = branch(c) * inverse * post_gain[...]
        out[c] = (residual_weight * tok[c].reshape(R, 256).astype(f32) + normed).astype(bf16)
        pltpu.make_async_copy(out.at[c], out_hbm.at[c], osem.at[0]).start()

    def scoped(stage, u):
        with jax.named_scope(stage.__name__):
            stage(u)

    to_add = LAGS[0]
    to_act = to_add + LAGS[1]
    to_pass = to_act + LAGS[2]
    to_down = to_pass + LAGS[3]
    to_z = to_down + LATER[0]
    to_x = to_z + LATER[1]
    to_end = to_x + LATER[2]

    def step(s, _):
        def at(stage, depth, ends=False):
            u = s - depth
            now = (u >= 0) & (u < 2 * C)
            if ends:
                now = now & (u >= G) & ((u < 2 * G) | (u % 2 == 1))
            pl.when(now)(lambda: scoped(stage, u))

        pl.when((s < 2 * C) & ((s < G) | ((s >= 2 * G) & (s % 2 == 0))))(lambda: arrived("xf", chunk_of(s)))
        pl.when(s == G)(lambda: have(wu.at[1], 1))
        at(up, 0)
        pl.when(s + G < early)(lambda: scoped(spread, s + G))
        at(add_up, to_add)
        pl.when(s == 2)(energy_over_y)
        pl.when(s == G - 2)(lambda: take(wu.at[1], 1))
        v = s - to_act
        pl.when((v < 2 * C) & (((v >= 0) & (v < G)) | ((v >= 2 * G) & (v % 2 == 0))))(lambda: turn(chunk_of(v)))
        at(activate, to_act)
        pl.when((s + 1 >= EAGER) & (s + 1 < G))(lambda: scoped(forward, s + 1))
        pl.when((s >= G) & (s < early))(lambda: scoped(forward, s))
        pl.when((s >= early + 3) & (s < C + 3))(lambda: scoped(forward, s - 3))
        pl.when((s >= early) & (s < C))(lambda: scoped(spread, s))
        at(pass_on, to_pass)
        pl.when(s == G + to_down - 1)(lambda: take(wd, 2))
        pl.when(s == G + to_down)(lambda: have(wd, 2))
        pl.when((s >= to_down) & (s < 2 * C + to_down))(lambda: arrived("a2", s - to_down))
        at(down, to_down, True)
        at(sum_z, to_z, True)
        at(sum_x, to_x, True)
        at(finish, to_end, True)
        return 0

    energy_over_z()
    lax.fori_loop(0, 2 * C + to_end, step, 0)
    with jax.named_scope("sent"):
        for name, total in sent.items():
            pltpu.make_async_copy(total, total, ssem.at[phases[name][0]]).wait()
        some = wu.at[0, 0:3, 0]
        for n, total in enumerate((some, some, wd.at[0:3, 0], some, some, wd.at[0:3, 0])):
            pltpu.make_async_copy(total, total, wssem.at[n]).wait()
        for n in range(2):
            pltpu.make_async_copy(e_in.at[n], e_in.at[n], esem.at[n]).wait()
        pltpu.make_async_copy(be_in, be_in, esem.at[4]).wait()
        pltpu.make_async_copy(out, out_hbm, osem.at[0]).wait()


def body(tokens, pre_gain, up_weight, up_bias, down_weight, post_gain):
    C = CHUNKS
    T = tokens.shape[0]
    R = T // C
    Q = R // 4
    hbm = pl.BlockSpec(memory_space=pl.ANY)
    dma = pltpu.SemaphoreType.DMA
    result = pl.pallas_call(
        kernel,
        out_shape=jax.ShapeDtypeStruct((C, R, 256), bf16),
        in_specs=[hbm] * 6,
        out_specs=hbm,
        scratch_shapes=[
            pltpu.VMEM((C, 4, Q, 256), bf16),
            pltpu.VMEM((1, 256), f32),
            pltpu.VMEM((4, 2, 1, 512), f32),
            pltpu.VMEM((1, 256), f32),
            pltpu.VMEM((C, 4, Q, 1024), bf16),
            pltpu.VMEM((2, 4, 2, 128, 512), bf16),
            pltpu.VMEM((4, 2, 512, 256), bf16),
            pltpu.VMEM((2 * C, 4, Q, 512), f32),
            pltpu.VMEM((2 * C, 4, Q, 512), bf16),
            pltpu.VMEM((2 * C, 2, Q, 256), bf16),
            pltpu.VMEM((2 * C, 2, Q, 256), bf16),
            pltpu.VMEM((2 * C, 2, Q, 512), bf16),
            pltpu.VMEM((2 * C, 4, Q, 512), bf16),
            pltpu.VMEM((C, 4, R, 256), bf16),
            pltpu.VMEM((C, 4, R, 256), f32),
            pltpu.VMEM((C, 3, R, 256), bf16),
            pltpu.VMEM((C, 4, R, 256), bf16),
            pltpu.VMEM((C, 1, R), f32),
            pltpu.VMEM((C, 4, Q, 8), f32),
            pltpu.VMEM((2, C, 1, R), f32),
            pltpu.VMEM((2, 3, C, 1, R), f32),
            pltpu.VMEM((C, 1, R), f32),
            pltpu.VMEM((C, 15, 1, R), f32),
            pltpu.VMEM((C, R, 256), bf16),
            dma((10,)),
            dma((5, C)),
            dma((2, 2 * C)),
            dma((5 + C,)),
            dma((6,)),
            dma((6, 3)),
            dma((10,)),
            dma((1,)),
        ],
        compiler_params=pltpu.CompilerParams(
            collective_id=0, has_side_effects=True, vmem_limit_bytes=VMEM_LIMIT
        ),
    )(
        tokens.reshape(C, 4, Q, 256),
        pre_gain.reshape(1, 256),
        up_bias.reshape(4, 2, 1, 512),
        post_gain.reshape(1, 256),
        up_weight,
        down_weight,
    )
    return result.reshape(T, 256)


def solution(mesh):
    in_specs = (P("dp", "ra"), P("ra"), P("ra", "cb"), P("cb"), P("cb", "ra"), P("ra"))
    out_specs = P("dp", "ra")
    return jax.shard_map(body, mesh=mesh, in_specs=in_specs, out_specs=out_specs, check_vma=False)
```

```python
import jax
import jax.numpy as jnp
from jax import lax
from jax.experimental import pallas as pl
from jax.experimental.pallas import tpu as pltpu
from jax.sharding import PartitionSpec as P

MESH = pl.DeviceIdType.MESH
D = 4096
CHUNKS = 12
GROUP = 5
FIRST = 5
AHEAD = 2
EAGER = 5
LAGS = (2, 2, 2, 2)
LATER = (4, 4, 6)
VMEM_LIMIT = 56 * 2**20
epsilon = 1e-06
residual_weight = 0.5
f32, bf16 = jnp.float32, jnp.bfloat16


def lane_sums_as_row(square):
    ones = jnp.ones((8, square.shape[1]), bf16)
    high = square.astype(bf16)
    low = (square - high.astype(f32)).astype(bf16)
    contract = (((1,), (1,)), ((), ()))
    total = lax.dot_general(ones, high, contract, preferred_element_type=f32)
    return total + lax.dot_general(ones, low, contract, preferred_element_type=f32)


def kernel(
    tok_hbm, pre_gain_hbm, up_bias_hbm, post_gain_hbm, up_hbm, down_hbm, out_hbm,
    tok, pre_gain, up_bias, post_gain, xg, wu, wd, pf, ps, r1, rs, pr, hg, os, of, zr, xa, inv_row, inv_col, e_own, e_in, be, be_in, out,
    ssem, csem, usem, esem, wssem, wrsem, hsem, lsem, osem,
):
    G = GROUP
    C, _, Q, _ = tok.shape
    R = 4 * Q
    ra, x, k = lax.axis_index("ra"), lax.axis_index("cb"), lax.axis_index("dp")
    z, y = ra // 4, ra % 4
    halves = (slice(0, 256), slice(256, 512))
    wide = (slice(0, 512), slice(512, 1024))

    def peer(axis, j):
        if axis == "r":
            return {"ra": (ra + j) % 16}
        if axis == "z":
            return {"ra": ((z + j) % 4) * 4 + y}
        if axis == "y":
            return {"ra": z * 4 + (y + j) % 4}
        if axis == "x":
            return {"cb": (x + j) % 4}
        return {"dp": 1 - k}

    def rdma(src, dst, ss, rs, axis, j):
        return pltpu.make_async_remote_copy(
            src_ref=src, dst_ref=dst, send_sem=ss, recv_sem=rs, device_id=peer(axis, j), device_id_type=MESH
        )

    def cols(at):
        return pl.ds(pl.multiple_of(at * 256, 256), 256)

    def side(j):
        return 0 if j == 1 else 1

    phases = {
        "xz": (0, "z", (1, 3, 2), lambda c, j: xg.at[c, x, :, cols(z)], lambda c, j: xg.at[c, x, :, cols(z)],
               lambda c: xa.at[c, 0:3, 0:Q]),
        "xx": (1, "x", (1, 3), lambda c, j: xg.at[c, x], lambda c, j: xg.at[c, x], lambda c: xg.at[c, 0:2]),
        "xf": (9, "x", (1, 3), lambda c, j: xg.at[c, (x + 4 - j) % 4, :, wide[side(j)]],
               lambda c, j: xg.at[c, (x + 4 - j) % 4, :, wide[side(j)]], lambda c: xg.at[c, 0]),
        "r1": (2, "y", (1, 3), lambda u, j: ps.at[u, (y + 2) % 4, :, halves[side(j)]], lambda u, j: r1.at[u, side(j)],
               lambda u: r1.at[u]),
        "rd": (3, "y", (1, 3), lambda u, j: ps.at[u, (y + j) % 4, :, halves[1 - side(j)]],
               lambda u, j: pr.at[u, side(j), :, halves[1 - side(j)]], lambda u: r1.at[u]),
        "r2": (4, "y", (1, 3), lambda u, j: rs.at[u, side(j)], lambda u, j: pr.at[u, side(j), :, halves[side(j)]],
               lambda u: pr.at[u]),
        "a1": (5, "y", (1, 3), lambda u, j: hg.at[u, y], lambda u, j: hg.at[u, y], lambda u: hg.at[u, 0:2]),
        "a2": (6, "y", (1, 3), lambda u, j: hg.at[u, (y + 4 - j) % 4, :, halves[side(j)]],
               lambda u, j: hg.at[u, (y + 4 - j) % 4, :, halves[side(j)]], lambda u: r1.at[u]),
        "zr": (7, "z", (2, 1, 3), lambda c, j: os.at[c, (z + j) % 4], lambda c, j: zr.at[c, j - 1], lambda c: zr.at[c]),
        "xa": (8, "x", (2, 1, 3), lambda c, j: xa.at[c, x], lambda c, j: xa.at[c, x], lambda c: zr.at[c]),
    }
    sent = {
        "xz": xa.at[:, 0:3, 0:Q], "xx": xg.at[:, 0:2], "xf": xg.at[:, 0], "r1": r1, "rd": r1, "r2": r1, "a1": hg.at[:, 0:2],
        "a2": r1, "zr": zr, "xa": zr,
    }
    by_chunk = {"xz": 0, "xx": 1, "zr": 2, "xa": 0, "xf": 3}
    by_unit = {"r1": 0, "rd": 1, "r2": 1, "a1": 0, "a2": 1}

    def landed(name, i):
        return csem.at[by_chunk[name], i] if name in by_chunk else usem.at[by_unit[name], i % 12]

    def send(name, i):
        n, axis, offsets, src, dst, _ = phases[name]
        for j in offsets:
            rdma(src(i, j), dst(i, j), ssem.at[n], landed(name, i), axis, j).start()

    def arrived(name, i):
        with jax.named_scope("wait_" + name):
            all_of_it = phases[name][5](i)
            pltpu.make_async_copy(all_of_it, all_of_it, landed(name, i)).wait()

    def up_block(h, j):
        at = pl.ds(pl.multiple_of(((z + j) % 4) * 1024 + h * 512, 512), 512)
        return rdma(
            up_hbm.at[pl.ds(pl.multiple_of(k * 128, 128), 128), at], wu.at[h, z, k], wssem.at[h], wrsem.at[h, j - 1], "z", j
        )

    def down_block(j):
        return rdma(
            down_hbm.at[pl.ds(pl.multiple_of(((z + j) % 4) * 1024 + k * 512, 512), 512), :],
            wd.at[z, k], wssem.at[2], wrsem.at[2, j - 1], "z", j,
        )

    def got(w, n, j):
        at = w.at[(z + 4 - j) % 4, k]
        return rdma(at, at, wssem.at[n], wrsem.at[n, j - 1], "z", j)

    def hand(w, n, j, half):
        at = w.at[(z + 4 - j) % 4, half]
        return rdma(at, at, wssem.at[n + 3], hsem.at[n], "k", 0)

    def take(w, n):
        with jax.named_scope("wait_w"):
            for j in (1, 3, 2):
                got(w, n, j).wait_recv()
                hand(w, n, j, k).start()

    def have(w, n):
        with jax.named_scope("wait_hand"):
            blocks = w.at[0:3, 0]
            pltpu.make_async_copy(blocks, blocks, hsem.at[n]).wait()

    def send_energy(n):
        for j in (1, 3, 2):
            rdma(e_own.at[n], e_in.at[n, j - 1], esem.at[n], esem.at[2 + n], "zy"[n], j).start()

    def have_energy(n):
        with jax.named_scope("wait_e"):
            pltpu.make_async_copy(e_in.at[n], e_in.at[n], esem.at[2 + n]).wait()
        return e_own[n] + e_in[n, 0] + e_in[n, 1] + e_in[n, 2]

    def send_rows(c):
        for j in range(1, 16):
            rdma(be.at[c], be_in.at[c, j - 1], esem.at[4], landed("xx", c), "r", j).start()

    barrier = pltpu.get_barrier_semaphore()
    partners = [(axis, j) for axis in "xyz" for j in (1, 2, 3)] + [("k", 0)]
    for axis, j in partners:
        pl.semaphore_signal(barrier, inc=1, device_id=peer(axis, j), device_id_type=MESH)

    load = pltpu.make_async_copy(tok_hbm, tok, lsem.at[0])
    load.start()
    small = []
    for n, (far, near) in enumerate(((pre_gain_hbm, pre_gain), (up_bias_hbm, up_bias), (post_gain_hbm, post_gain))):
        small.append(pltpu.make_async_copy(far, near, lsem.at[1 + n]))
        small[-1].start()
    own = []
    for half in range(2):
        for h in range(2):
            own.append(pltpu.make_async_copy(
                up_hbm.at[pl.ds(half * 128, 128), pl.ds(pl.multiple_of(z * 1024 + h * 512, 512), 512)],
                wu.at[h, z, half], lsem.at[4]))
        own.append(pltpu.make_async_copy(
            down_hbm.at[pl.ds(pl.multiple_of(z * 1024 + half * 512, 512), 512), :], wd.at[z, half], lsem.at[5]))
    for o in own:
        o.start()
    load.wait()
    for o in small:
        o.wait()

    gain = pre_gain[...]

    def scale(c, _):
        xg[c, x, :, cols(z)] = (tok[c, x].astype(f32) * gain).astype(bf16)
        return 0

    def own_energy(c, _):
        part = tok[c].reshape(R, 256).astype(f32)
        e_own[0, c] = lane_sums_as_row(part * part)[0:1]
        return 0

    with jax.named_scope("scale"):
        lax.fori_loop(0, C, scale, 0)
    with jax.named_scope("wait_barrier"):
        pl.semaphore_wait(barrier, len(partners))

    early = max(G, C // 2)
    for c in range(FIRST):
        send("xz", c)
    for j in (1, 3, 2):
        up_block(0, j).start()
    with jax.named_scope("own_energy"):
        lax.fori_loop(0, C, own_energy, 0)
    send_energy(0)
    for c in range(FIRST, early):
        send("xz", c)
    for j in (1, 3, 2):
        up_block(1, j).start()
    lax.fori_loop(early, C, lambda c, _: (send("xz", c), 0)[1], 0)
    for j in (1, 3, 2):
        down_block(j).start()

    def spread(c):
        arrived("xz", c)
        send("xx", c)

    def forward(c):
        arrived("xx", c)
        send("xf", c)

    for c in range(FIRST):
        spread(c)
    for c in range(AHEAD):
        forward(c)
    take(wu.at[0], 0)
    for c in range(FIRST, G):
        spread(c)
    for c in range(AHEAD, EAGER):
        forward(c)
    for n, blocks in ((4, wu.at[:, 0]), (5, wd.at[0])):
        pltpu.make_async_copy(blocks, blocks, lsem.at[n]).wait()
    have(wu.at[0], 0)

    def energy_over_z():
        e_own[1] = have_energy(0)
        send_energy(1)

    def energy_over_y():
        inv_row[...] = lax.rsqrt(have_energy(1) / D + epsilon)


    def turn(c):
        inv_col[c] = jnp.transpose(jnp.broadcast_to(inv_row[c], (8, R))).reshape(4, Q, 8)

    def late(u):
        return (u // (2 * G) + 15) // 16

    def chunk_of(u):
        return late(u) * (u // 2) + (1 - late(u)) * (u % G)

    def half_of(u):
        return late(u) * (u % 2) + (1 - late(u)) * (u // G)

    def up(u):
        c, h = chunk_of(u), half_of(u)
        rows = xg[c].reshape(R, 1024)
        for n in range(2):
            at = slice(n * 256, (n + 1) * 256)
            part = jnp.dot(rows, wu[h, :, :, :, at].reshape(1024, 256), preferred_element_type=f32).reshape(4, Q, 256)
            pf[u, :, :, at] = part
            ps[u, :, :, at] = part.astype(bf16)
        send("r1", u)
        send("rd", u)

    def add_up(u):
        arrived("r1", u)
        for j in (1, 3):
            n = side(j)
            rs[u, n] = (pf[u, (y + j) % 4, :, halves[n]] + r1[u, n].astype(f32)).astype(bf16)
        send("r2", u)

    def activate(u):
        arrived("r2", u)
        inverse = inv_col[chunk_of(u), y][:, 0:1]
        pre = pf[u, y] + pr[u, 0].astype(f32) + pr[u, 1].astype(f32)
        pre = pre * inverse + up_bias[z, half_of(u)]
        hg[u, y] = jnp.square(jnp.maximum(pre, 0.0)).astype(bf16)
        send("a1", u)

    def pass_on(u):
        arrived("a1", u)
        send("a2", u)

    def last_of(u):
        return late(u) * ((u - 1) // 2) + (1 - late(u)) * (u - G)

    def down(u):
        c = last_of(u)
        other = late(u) * (u - 1) + (1 - late(u)) * (u - G)
        for n in range(4):
            part = jnp.dot(hg[other].reshape(R, 512), wd[n, 0], preferred_element_type=f32)
            part = part + jnp.dot(hg[u].reshape(R, 512), wd[n, 1], preferred_element_type=f32)
            of[c, n] = part
            os[c, n] = part.astype(bf16)
        send("zr", c)

    def sum_z(u):
        c = last_of(u)
        arrived("zr", c)
        total = of[c, z]
        for j in range(3):
            total = total + zr[c, j].astype(f32)
        xa[c, x] = total.astype(bf16)
        send("xa", c)

    def branch(c):
        return (xa[c, 0].astype(f32) + xa[c, 1].astype(f32)) + (xa[c, 2].astype(f32) + xa[c, 3].astype(f32))

    def sum_x(u):
        c = last_of(u)
        arrived("xa", c)
        total = branch(c)
        be[c] = lane_sums_as_row(total * total)[0:1]
        send_rows(c)

    def finish(u):
        c = last_of(u)
        with jax.named_scope("wait_be"):
            pltpu.make_async_copy(be_in.at[c], be_in.at[c], landed("xx", c)).wait()
        total = be[c]
        for j in range(15):
            total = total + be_in[c, j]
        inverse = jnp.transpose(jnp.broadcast_to(lax.rsqrt(total / D + epsilon), (8, R)))[:, 0:1]
        normed = branch(c) * inverse * post_gain[...]
        out[c] = (residual_weight * tok[c].reshape(R, 256).astype(f32) + normed).astype(bf16)
        pltpu.make_async_copy(out.at[c], out_hbm.at[c], osem.at[0]).start()

    def scoped(stage, u):
        with jax.named_scope(stage.__name__):
            stage(u)

    to_add = LAGS[0]
    to_act = to_add + LAGS[1]
    to_pass = to_act + LAGS[2]
    to_down = to_pass + LAGS[3]
    to_z = to_down + LATER[0]
    to_x = to_z + LATER[1]
    to_end = to_x + LATER[2]

    def step(s, _):
        def at(stage, depth, ends=False):
            u = s - depth
            now = (u >= 0) & (u < 2 * C)
            if ends:
                now = now & (u >= G) & ((u < 2 * G) | (u % 2 == 1))
            pl.when(now)(lambda: scoped(stage, u))

        pl.when((s < 2 * C) & ((s < G) | ((s >= 2 * G) & (s % 2 == 0))))(lambda: arrived("xf", chunk_of(s)))
        pl.when(s == G)(lambda: have(wu.at[1], 1))
        at(up, 0)
        pl.when(s + G < early)(lambda: scoped(spread, s + G))
        at(add_up, to_add)
        pl.when(s == 2)(energy_over_y)
        pl.when(s == G - 2)(lambda: take(wu.at[1], 1))
        v = s - to_act
        pl.when((v < 2 * C) & (((v >= 0) & (v < G)) | ((v >= 2 * G) & (v % 2 == 0))))(lambda: turn(chunk_of(v)))
        at(activate, to_act)
        pl.when((s + 1 >= EAGER) & (s + 1 < G))(lambda: scoped(forward, s + 1))
        pl.when((s >= G) & (s < early))(lambda: scoped(forward, s))
        pl.when((s >= early + 3) & (s < C + 3))(lambda: scoped(forward, s - 3))
        pl.when((s >= early) & (s < C))(lambda: scoped(spread, s))
        at(pass_on, to_pass)
        pl.when(s == G + to_down - 1)(lambda: take(wd, 2))
        pl.when(s == G + to_down)(lambda: have(wd, 2))
        pl.when((s >= to_down) & (s < 2 * C + to_down))(lambda: arrived("a2", s - to_down))
        at(down, to_down, True)
        at(sum_z, to_z, True)
        at(sum_x, to_x, True)
        at(finish, to_end, True)
        return 0

    energy_over_z()
    lax.fori_loop(0, 2 * C + to_end, step, 0)
    with jax.named_scope("sent"):
        for name, total in sent.items():
            pltpu.make_async_copy(total, total, ssem.at[phases[name][0]]).wait()
        some = wu.at[0, 0:3, 0]
        for n, total in enumerate((some, some, wd.at[0:3, 0], some, some, wd.at[0:3, 0])):
            pltpu.make_async_copy(total, total, wssem.at[n]).wait()
        for n in range(2):
            pltpu.make_async_copy(e_in.at[n], e_in.at[n], esem.at[n]).wait()
        pltpu.make_async_copy(be_in, be_in, esem.at[4]).wait()
        pltpu.make_async_copy(out, out_hbm, osem.at[0]).wait()


def body(tokens, pre_gain, up_weight, up_bias, down_weight, post_gain):
    C = CHUNKS
    T = tokens.shape[0]
    R = T // C
    Q = R // 4
    hbm = pl.BlockSpec(memory_space=pl.ANY)
    dma = pltpu.SemaphoreType.DMA
    result = pl.pallas_call(
        kernel,
        out_shape=jax.ShapeDtypeStruct((C, R, 256), bf16),
        in_specs=[hbm] * 6,
        out_specs=hbm,
        scratch_shapes=[
            pltpu.VMEM((C, 4, Q, 256), bf16),
            pltpu.VMEM((1, 256), f32),
            pltpu.VMEM((4, 2, 1, 512), f32),
            pltpu.VMEM((1, 256), f32),
            pltpu.VMEM((C, 4, Q, 1024), bf16),
            pltpu.VMEM((2, 4, 2, 128, 512), bf16),
            pltpu.VMEM((4, 2, 512, 256), bf16),
            pltpu.VMEM((2 * C, 4, Q, 512), f32),
            pltpu.VMEM((2 * C, 4, Q, 512), bf16),
            pltpu.VMEM((2 * C, 2, Q, 256), bf16),
            pltpu.VMEM((2 * C, 2, Q, 256), bf16),
            pltpu.VMEM((2 * C, 2, Q, 512), bf16),
            pltpu.VMEM((2 * C, 4, Q, 512), bf16),
            pltpu.VMEM((C, 4, R, 256), bf16),
            pltpu.VMEM((C, 4, R, 256), f32),
            pltpu.VMEM((C, 3, R, 256), bf16),
            pltpu.VMEM((C, 4, R, 256), bf16),
            pltpu.VMEM((C, 1, R), f32),
            pltpu.VMEM((C, 4, Q, 8), f32),
            pltpu.VMEM((2, C, 1, R), f32),
            pltpu.VMEM((2, 3, C, 1, R), f32),
            pltpu.VMEM((C, 1, R), f32),
            pltpu.VMEM((C, 15, 1, R), f32),
            pltpu.VMEM((C, R, 256), bf16),
            dma((10,)),
            dma((4, C)),
            dma((2, 12)),
            dma((5,)),
            dma((6,)),
            dma((3, 3)),
            dma((3,)),
            dma((6,)),
            dma((1,)),
        ],
        compiler_params=pltpu.CompilerParams(
            collective_id=0, has_side_effects=True, vmem_limit_bytes=VMEM_LIMIT
        ),
    )(
        tokens.reshape(C, 4, Q, 256),
        pre_gain.reshape(1, 256),
        up_bias.reshape(4, 2, 1, 512),
        post_gain.reshape(1, 256),
        up_weight,
        down_weight,
    )
    return result.reshape(T, 256)


def solution(mesh):
    in_specs = (P("dp", "ra"), P("ra"), P("ra", "cb"), P("cb"), P("cb", "ra"), P("ra"))
    out_specs = P("dp", "ra")
    return jax.shard_map(body, mesh=mesh, in_specs=in_specs, out_specs=out_specs, check_vma=False)
```

```python
import jax
import jax.numpy as jnp
from jax import lax
from jax.experimental import pallas as pl
from jax.experimental.pallas import tpu as pltpu
from jax.sharding import PartitionSpec as P

MESH = pl.DeviceIdType.MESH
D = 4096
CHUNKS = 12
GROUP = 5
FIRST = 5
AHEAD = 2
EAGER = 5
LAGS = (2, 2, 2, 2)
LATER = (4, 4, 6)
VMEM_LIMIT = 56 * 2**20
epsilon = 1e-06
residual_weight = 0.5
f32, bf16 = jnp.float32, jnp.bfloat16


def lane_sums_as_row(square):
    ones = jnp.ones((8, square.shape[1]), bf16)
    high = square.astype(bf16)
    low = (square - high.astype(f32)).astype(bf16)
    contract = (((1,), (1,)), ((), ()))
    total = lax.dot_general(ones, high, contract, preferred_element_type=f32)
    return total + lax.dot_general(ones, low, contract, preferred_element_type=f32)


def kernel(
    tok_hbm, pre_gain_hbm, up_bias_hbm, post_gain_hbm, up_hbm, down_hbm, out_hbm,
    tok, pre_gain, up_bias, post_gain, xg, wu, wd, pf, ps, r1, rs, pr, hg, os, of, zr, xa, inv_row, inv_col, e_own, e_in, be, be_in, out,
    ssem, csem, usem, esem, wssem, wrsem, hsem, lsem, osem,
):
    G = GROUP
    C, _, Q, _ = tok.shape
    R = 4 * Q
    ra, x, k = lax.axis_index("ra"), lax.axis_index("cb"), lax.axis_index("dp")
    z, y = ra // 4, ra % 4
    halves = (slice(0, 256), slice(256, 512))
    wide = (slice(0, 512), slice(512, 1024))

    def peer(axis, j):
        if axis == "r":
            return {"ra": (ra + j) % 16}
        if axis == "z":
            return {"ra": ((z + j) % 4) * 4 + y}
        if axis == "y":
            return {"ra": z * 4 + (y + j) % 4}
        if axis == "x":
            return {"cb": (x + j) % 4}
        return {"dp": 1 - k}

    def rdma(src, dst, ss, rs, axis, j):
        return pltpu.make_async_remote_copy(
            src_ref=src, dst_ref=dst, send_sem=ss, recv_sem=rs, device_id=peer(axis, j), device_id_type=MESH
        )

    def cols(at):
        return pl.ds(pl.multiple_of(at * 256, 256), 256)

    def side(j):
        return 0 if j == 1 else 1

    phases = {
        "xz": (0, "z", (1, 3, 2), lambda c, j: xg.at[c, x, :, cols(z)], lambda c, j: xg.at[c, x, :, cols(z)],
               lambda c: xa.at[c, 0:3, 0:Q]),
        "xx": (1, "x", (1, 3), lambda c, j: xg.at[c, x], lambda c, j: xg.at[c, x], lambda c: xg.at[c, 0:2]),
        "xf": (9, "x", (1, 3), lambda c, j: xg.at[c, (x + 4 - j) % 4, :, wide[side(j)]],
               lambda c, j: xg.at[c, (x + 4 - j) % 4, :, wide[side(j)]], lambda c: xg.at[c, 0]),
        "r1": (2, "y", (1, 3), lambda u, j: ps.at[u, (y + 2) % 4, :, halves[side(j)]], lambda u, j: r1.at[u, side(j)],
               lambda u: r1.at[u]),
        "rd": (3, "y", (1, 3), lambda u, j: ps.at[u, (y + j) % 4, :, halves[1 - side(j)]],
               lambda u, j: pr.at[u, side(j), :, halves[1 - side(j)]], lambda u: r1.at[u]),
        "r2": (4, "y", (1, 3), lambda u, j: rs.at[u, side(j)], lambda u, j: pr.at[u, side(j), :, halves[side(j)]],
               lambda u: pr.at[u]),
        "a1": (5, "y", (1, 3), lambda u, j: hg.at[u, y], lambda u, j: hg.at[u, y], lambda u: hg.at[u, 0:2]),
        "a2": (6, "y", (1, 3), lambda u, j: hg.at[u, (y + 4 - j) % 4, :, halves[side(j)]],
               lambda u, j: hg.at[u, (y + 4 - j) % 4, :, halves[side(j)]], lambda u: r1.at[u]),
        "zr": (7, "z", (2, 1, 3), lambda c, j: os.at[c, (z + j) % 4], lambda c, j: zr.at[c, j - 1], lambda c: zr.at[c]),
        "xa": (8, "x", (2, 1, 3), lambda c, j: xa.at[c, x], lambda c, j: xa.at[c, x], lambda c: zr.at[c]),
    }
    sent = {
        "xz": xa.at[:, 0:3, 0:Q], "xx": xg.at[:, 0:2], "xf": xg.at[:, 0], "r1": r1, "rd": r1, "r2": r1, "a1": hg.at[:, 0:2],
        "a2": r1, "zr": zr, "xa": zr,
    }
    by_chunk = {"xz": 0, "xx": 1, "zr": 2, "xa": 0, "xf": 3}
    by_unit = {"r1": 0, "rd": 1, "r2": 1, "a1": 0, "a2": 1}

    def landed(name, i):
        return csem.at[by_chunk[name], i] if name in by_chunk else usem.at[by_unit[name], i % 12]

    def send(name, i):
        n, axis, offsets, src, dst, _ = phases[name]
        for j in offsets:
            rdma(src(i, j), dst(i, j), ssem.at[n], landed(name, i), axis, j).start()

    def arrived(name, i):
        with jax.named_scope("wait_" + name):
            all_of_it = phases[name][5](i)
            pltpu.make_async_copy(all_of_it, all_of_it, landed(name, i)).wait()

    def up_block(h, j):
        at = pl.ds(pl.multiple_of(((z + j) % 4) * 1024 + h * 512, 512), 512)
        return rdma(
            up_hbm.at[pl.ds(pl.multiple_of(k * 128, 128), 128), at], wu.at[h, z, k], wssem.at[h], wrsem.at[h, j - 1], "z", j
        )

    def down_block(j):
        return rdma(
            down_hbm.at[pl.ds(pl.multiple_of(((z + j) % 4) * 1024 + k * 512, 512), 512), :],
            wd.at[z, k], wssem.at[2], wrsem.at[2, j - 1], "z", j,
        )

    def got(w, n, j):
        at = w.at[(z + 4 - j) % 4, k]
        return rdma(at, at, wssem.at[n], wrsem.at[n, j - 1], "z", j)

    def hand(w, n, j, half):
        at = w.at[(z + 4 - j) % 4, half]
        return rdma(at, at, wssem.at[n + 3], hsem.at[n], "k", 0)

    def take(w, n):
        with jax.named_scope("wait_w"):
            for j in (1, 3, 2):
                got(w, n, j).wait_recv()
                hand(w, n, j, k).start()

    def have(w, n):
        with jax.named_scope("wait_hand"):
            blocks = w.at[0:3, 0]
            pltpu.make_async_copy(blocks, blocks, hsem.at[n]).wait()

    def send_energy(n):
        for j in (1, 3, 2):
            rdma(e_own.at[n], e_in.at[n, j - 1], esem.at[n], esem.at[2 + n], "zy"[n], j).start()

    def have_energy(n):
        with jax.named_scope("wait_e"):
            pltpu.make_async_copy(e_in.at[n], e_in.at[n], esem.at[2 + n]).wait()
        return e_own[n] + e_in[n, 0] + e_in[n, 1] + e_in[n, 2]

    def send_rows(c):
        for j in range(1, 16):
            rdma(be.at[c], be_in.at[c, j - 1], esem.at[4], landed("xx", c), "r", j).start()

    barrier = pltpu.get_barrier_semaphore()
    partners = [(axis, j) for axis in "xyz" for j in (1, 2, 3)] + [("k", 0)]
    for axis, j in partners:
        pl.semaphore_signal(barrier, inc=1, device_id=peer(axis, j), device_id_type=MESH)

    load = pltpu.make_async_copy(tok_hbm.at[:, x], tok.at[:, x], lsem.at[0])
    load.start()
    small = []
    for n, (far, near) in enumerate(((pre_gain_hbm, pre_gain), (up_bias_hbm, up_bias), (post_gain_hbm, post_gain))):
        small.append(pltpu.make_async_copy(far, near, lsem.at[1 + n]))
        small[-1].start()
    own = []
    for half in range(2):
        for h in range(2):
            own.append(pltpu.make_async_copy(
                up_hbm.at[pl.ds(half * 128, 128), pl.ds(pl.multiple_of(z * 1024 + h * 512, 512), 512)],
                wu.at[h, z, half], lsem.at[4]))
        own.append(pltpu.make_async_copy(
            down_hbm.at[pl.ds(pl.multiple_of(z * 1024 + half * 512, 512), 512), :], wd.at[z, half], lsem.at[5]))
    small[0].wait()
    load.wait()
    for j in (1, 2, 3):
        at = (x + j) % 4
        pltpu.make_async_copy(tok_hbm.at[:, at], tok.at[:, at], lsem.at[6]).start()
    for o in own:
        o.start()
    for o in small[1:]:
        o.wait()

    gain = pre_gain[...]

    def scale(c, _):
        xg[c, x, :, cols(z)] = (tok[c, x].astype(f32) * gain).astype(bf16)
        return 0

    def own_energy(c, _):
        part = tok[c].reshape(R, 256).astype(f32)
        e_own[0, c] = lane_sums_as_row(part * part)[0:1]
        return 0

    with jax.named_scope("scale"):
        lax.fori_loop(0, C, scale, 0)
    with jax.named_scope("wait_barrier"):
        pl.semaphore_wait(barrier, len(partners))

    early = max(G, C // 2)
    for c in range(FIRST):
        send("xz", c)
    for j in (1, 3, 2):
        up_block(0, j).start()
    with jax.named_scope("own_energy"):
        others = tok.at[:, 0:3]
        pltpu.make_async_copy(others, others, lsem.at[6]).wait()
        lax.fori_loop(0, C, own_energy, 0)
    send_energy(0)
    for c in range(FIRST, early):
        send("xz", c)
    for j in (1, 3, 2):
        up_block(1, j).start()
    lax.fori_loop(early, C, lambda c, _: (send("xz", c), 0)[1], 0)
    for j in (1, 3, 2):
        down_block(j).start()

    def spread(c):
        arrived("xz", c)
        send("xx", c)

    def forward(c):
        arrived("xx", c)
        send("xf", c)

    for c in range(FIRST):
        spread(c)
    for c in range(AHEAD):
        forward(c)
    take(wu.at[0], 0)
    for c in range(FIRST, G):
        spread(c)
    for c in range(AHEAD, EAGER):
        forward(c)
    for n, blocks in ((4, wu.at[:, 0]), (5, wd.at[0])):
        pltpu.make_async_copy(blocks, blocks, lsem.at[n]).wait()
    have(wu.at[0], 0)

    def energy_over_z():
        e_own[1] = have_energy(0)
        send_energy(1)

    def energy_over_y():
        inv_row[...] = lax.rsqrt(have_energy(1) / D + epsilon)


    def turn(c):
        inv_col[c] = jnp.transpose(jnp.broadcast_to(inv_row[c], (8, R))).reshape(4, Q, 8)

    def late(u):
        return (u // (2 * G) + 15) // 16

    def chunk_of(u):
        return late(u) * (u // 2) + (1 - late(u)) * (u % G)

    def half_of(u):
        return late(u) * (u % 2) + (1 - late(u)) * (u // G)

    def up(u):
        c, h = chunk_of(u), half_of(u)
        rows = xg[c].reshape(R, 1024)
        for n in range(2):
            at = slice(n * 256, (n + 1) * 256)
            part = jnp.dot(rows, wu[h, :, :, :, at].reshape(1024, 256), preferred_element_type=f32).reshape(4, Q, 256)
            pf[u, :, :, at] = part
            ps[u, :, :, at] = part.astype(bf16)
        send("r1", u)
        send("rd", u)

    def add_up(u):
        arrived("r1", u)
        for j in (1, 3):
            n = side(j)
            rs[u, n] = (pf[u, (y + j) % 4, :, halves[n]] + r1[u, n].astype(f32)).astype(bf16)
        send("r2", u)

    def activate(u):
        arrived("r2", u)
        inverse = inv_col[chunk_of(u), y][:, 0:1]
        pre = pf[u, y] + pr[u, 0].astype(f32) + pr[u, 1].astype(f32)
        pre = pre * inverse + up_bias[z, half_of(u)]
        hg[u, y] = jnp.square(jnp.maximum(pre, 0.0)).astype(bf16)
        send("a1", u)

    def pass_on(u):
        arrived("a1", u)
        send("a2", u)

    def last_of(u):
        return late(u) * ((u - 1) // 2) + (1 - late(u)) * (u - G)

    def down(u):
        c = last_of(u)
        other = late(u) * (u - 1) + (1 - late(u)) * (u - G)
        for n in range(4):
            part = jnp.dot(hg[other].reshape(R, 512), wd[n, 0], preferred_element_type=f32)
            part = part + jnp.dot(hg[u].reshape(R, 512), wd[n, 1], preferred_element_type=f32)
            of[c, n] = part
            os[c, n] = part.astype(bf16)
        send("zr", c)

    def sum_z(u):
        c = last_of(u)
        arrived("zr", c)
        total = of[c, z]
        for j in range(3):
            total = total + zr[c, j].astype(f32)
        xa[c, x] = total.astype(bf16)
        send("xa", c)

    def branch(c):
        return (xa[c, 0].astype(f32) + xa[c, 1].astype(f32)) + (xa[c, 2].astype(f32) + xa[c, 3].astype(f32))

    def sum_x(u):
        c = last_of(u)
        arrived("xa", c)
        total = branch(c)
        be[c] = lane_sums_as_row(total * total)[0:1]
        send_rows(c)

    def finish(u):
        c = last_of(u)
        with jax.named_scope("wait_be"):
            pltpu.make_async_copy(be_in.at[c], be_in.at[c], landed("xx", c)).wait()
        total = be[c]
        for j in range(15):
            total = total + be_in[c, j]
        inverse = jnp.transpose(jnp.broadcast_to(lax.rsqrt(total / D + epsilon), (8, R)))[:, 0:1]
        normed = branch(c) * inverse * post_gain[...]
        out[c] = (residual_weight * tok[c].reshape(R, 256).astype(f32) + normed).astype(bf16)
        pltpu.make_async_copy(out.at[c], out_hbm.at[c], osem.at[0]).start()

    def scoped(stage, u):
        with jax.named_scope(stage.__name__):
            stage(u)

    to_add = LAGS[0]
    to_act = to_add + LAGS[1]
    to_pass = to_act + LAGS[2]
    to_down = to_pass + LAGS[3]
    to_z = to_down + LATER[0]
    to_x = to_z + LATER[1]
    to_end = to_x + LATER[2]

    def step(s, _):
        def at(stage, depth, ends=False):
            u = s - depth
            now = (u >= 0) & (u < 2 * C)
            if ends:
                now = now & (u >= G) & ((u < 2 * G) | (u % 2 == 1))
            pl.when(now)(lambda: scoped(stage, u))

        pl.when((s < 2 * C) & ((s < G) | ((s >= 2 * G) & (s % 2 == 0))))(lambda: arrived("xf", chunk_of(s)))
        pl.when(s == G)(lambda: have(wu.at[1], 1))
        at(up, 0)
        pl.when(s + G < early)(lambda: scoped(spread, s + G))
        at(add_up, to_add)
        pl.when(s == 2)(energy_over_y)
        pl.when(s == G - 2)(lambda: take(wu.at[1], 1))
        v = s - to_act
        pl.when((v < 2 * C) & (((v >= 0) & (v < G)) | ((v >= 2 * G) & (v % 2 == 0))))(lambda: turn(chunk_of(v)))
        at(activate, to_act)
        pl.when((s + 1 >= EAGER) & (s + 1 < G))(lambda: scoped(forward, s + 1))
        pl.when((s >= G) & (s < early))(lambda: scoped(forward, s))
        pl.when((s >= early + 3) & (s < C + 3))(lambda: scoped(forward, s - 3))
        pl.when((s >= early) & (s < C))(lambda: scoped(spread, s))
        at(pass_on, to_pass)
        pl.when(s == G + to_down - 1)(lambda: take(wd, 2))
        pl.when(s == G + to_down)(lambda: have(wd, 2))
        pl.when((s >= to_down) & (s < 2 * C + to_down))(lambda: arrived("a2", s - to_down))
        at(down, to_down, True)
        at(sum_z, to_z, True)
        at(sum_x, to_x, True)
        at(finish, to_end, True)
        return 0

    energy_over_z()
    lax.fori_loop(0, 2 * C + to_end, step, 0)
    with jax.named_scope("sent"):
        for name, total in sent.items():
            pltpu.make_async_copy(total, total, ssem.at[phases[name][0]]).wait()
        some = wu.at[0, 0:3, 0]
        for n, total in enumerate((some, some, wd.at[0:3, 0], some, some, wd.at[0:3, 0])):
            pltpu.make_async_copy(total, total, wssem.at[n]).wait()
        for n in range(2):
            pltpu.make_async_copy(e_in.at[n], e_in.at[n], esem.at[n]).wait()
        pltpu.make_async_copy(be_in, be_in, esem.at[4]).wait()
        pltpu.make_async_copy(out, out_hbm, osem.at[0]).wait()


def body(tokens, pre_gain, up_weight, up_bias, down_weight, post_gain):
    C = CHUNKS
    T = tokens.shape[0]
    R = T // C
    Q = R // 4
    hbm = pl.BlockSpec(memory_space=pl.ANY)
    dma = pltpu.SemaphoreType.DMA
    result = pl.pallas_call(
        kernel,
        out_shape=jax.ShapeDtypeStruct((C, R, 256), bf16),
        in_specs=[hbm] * 6,
        out_specs=hbm,
        scratch_shapes=[
            pltpu.VMEM((C, 4, Q, 256), bf16),
            pltpu.VMEM((1, 256), f32),
            pltpu.VMEM((4, 2, 1, 512), f32),
            pltpu.VMEM((1, 256), f32),
            pltpu.VMEM((C, 4, Q, 1024), bf16),
            pltpu.VMEM((2, 4, 2, 128, 512), bf16),
            pltpu.VMEM((4, 2, 512, 256), bf16),
            pltpu.VMEM((2 * C, 4, Q, 512), f32),
            pltpu.VMEM((2 * C, 4, Q, 512), bf16),
            pltpu.VMEM((2 * C, 2, Q, 256), bf16),
            pltpu.VMEM((2 * C, 2, Q, 256), bf16),
            pltpu.VMEM((2 * C, 2, Q, 512), bf16),
            pltpu.VMEM((2 * C, 4, Q, 512), bf16),
            pltpu.VMEM((C, 4, R, 256), bf16),
            pltpu.VMEM((C, 4, R, 256), f32),
            pltpu.VMEM((C, 3, R, 256), bf16),
            pltpu.VMEM((C, 4, R, 256), bf16),
            pltpu.VMEM((C, 1, R), f32),
            pltpu.VMEM((C, 4, Q, 8), f32),
            pltpu.VMEM((2, C, 1, R), f32),
            pltpu.VMEM((2, 3, C, 1, R), f32),
            pltpu.VMEM((C, 1, R), f32),
            pltpu.VMEM((C, 15, 1, R), f32),
            pltpu.VMEM((C, R, 256), bf16),
            dma((10,)),
            dma((4, C)),
            dma((2, 12)),
            dma((5,)),
            dma((6,)),
            dma((3, 3)),
            dma((3,)),
            dma((7,)),
            dma((1,)),
        ],
        compiler_params=pltpu.CompilerParams(
            collective_id=0, has_side_effects=True, vmem_limit_bytes=VMEM_LIMIT
        ),
    )(
        tokens.reshape(C, 4, Q, 256),
        pre_gain.reshape(1, 256),
        up_bias.reshape(4, 2, 1, 512),
        post_gain.reshape(1, 256),
        up_weight,
        down_weight,
    )
    return result.reshape(T, 256)


def solution(mesh):
    in_specs = (P("dp", "ra"), P("ra"), P("ra", "cb"), P("cb"), P("cb", "ra"), P("ra"))
    out_specs = P("dp", "ra")
    return jax.shard_map(body, mesh=mesh, in_specs=in_specs, out_specs=out_specs, check_vma=False)
```
